32 devices in a mesh: ep: 8 (over z, core), tp: 4 (over y, x).
Axes of the slice: x: 2, y: 2, z: 4, core: 2. Of those that a mesh axis runs over, the one named last changes fastest.
Arguments:
- tokens: bfloat16 [128, 4096], P('ep', 'tp'), may hold values from -40 to 40
- norm_gain: bfloat16 [4096], P('tp'), may hold values from 0.099609375 to 1.8984375
- routes: int32 [128, 4], P('ep'), may hold values from 0 to 7, all different within a row; in each aligned block of 16 rows (0 to 15, 16 to 31, ...) at most 16 rows name the same one
- route_weights: float32 [128, 4], P('ep'), may hold values from 0.05 to 1
- w_gate: bfloat16 [8, 4096, 4096], P('ep', None, 'tp'), may hold values from -0.25 to 0.25
- w_up: bfloat16 [8, 4096, 4096], P('ep', None, 'tp'), may hold values from -0.25 to 0.25
- w_down: bfloat16 [8, 4096, 4096], P('ep', 'tp'), may hold values from -0.0234375 to 0.0234375
Outputs:
- mixed: bfloat16 [128, 4096], P('ep', 'tp')
The draws below stay inside these ranges and needn't reach their ends.
Inputs may be any that keep to these rules, and one draw needn't show every extreme that they name: `routes`: within the 16 rows of one device, each token names 4 different experts, and no expert is named by more than 16 rows; some expert reaches 16.
All inputs are finite; a program needn't handle non-finite values.
Results may differ from the reference program's by a relative error of at most 0.018.
Values may be sent and summed in bfloat16 or wider, within the bound.
No kernel may reach another device: no remote copies, remote signals or barrier semaphores. Data moves between devices by JAX's collectives and lax.ppermute only.
A program may use at most 64 MiB of HBM per device.

```python
import math
import jax
import jax.numpy as jnp
import numpy as np
from jax import lax

D = 4096
FF = 4096
TOPK = 4
TOK_DEV = 16
EXPERTS = 8
CAP = 16
TOKENS = 128
N_TP = 4


def draw_tokens(key, part):
    first, second, third = jax.random.split(key, 3)
    blocks = max(D // 128, 1)
    width = D // blocks
    column_scale = jnp.exp(jax.random.uniform(second, (blocks,), jnp.float32, -1.1, 1.1))
    column_scale = jnp.repeat(column_scale, width)
    values = jax.random.normal(first, (TOKENS, D), jnp.float32) * column_scale[None, :]
    return jnp.clip(values, -40.0, 40.0).astype(jnp.bfloat16)


def level_of(stream_key, extent, cuts, smallest, top_value):
    level, own = 1.0, jax.random.fold_in(stream_key, 6)
    for axis_at, shards_of in cuts:
        heights = jnp.exp(jax.random.uniform(jax.random.fold_in(own, axis_at), (shards_of,), jnp.float32, smallest / len(cuts), top_value / len(cuts)))
        level = level * jnp.repeat(heights, extent[axis_at] // shards_of).reshape([-1 if axis == axis_at else 1 for axis in range(len(extent))])
    return level


def assign_block(rng, own, number, rows, number_of, top, bound, lean):
    sequence = jax.random.permutation(rng, number_of)
    heavy_load, usual = shares(number_of, rows * top, bound, lean, True), shares(number_of, rows * top, bound, lean, False)
    places = jnp.arange(number_of)

    def named(tallies, turn):
        used = int((tallies > 0).sum())
        fixed = max(1, used // 4)
        moved = fixed + (places - fixed + turn * (used - fixed)) % max(1, number_of - fixed)
        return jnp.zeros((number_of,), jnp.int32).at[sequence[jnp.where(places < fixed, places, moved)]].set(jnp.asarray(tallies, jnp.int32))

    tallies = jnp.where(number % 4 == 0, named(heavy_load, number // 4), named(usual, number - number // 4 - 1))
    mixed = jax.random.permutation(jax.random.fold_in(own, 3), number_of)
    giver, sink = mixed[0:number_of // 2 * 2:2], mixed[1:number_of // 2 * 2:2]
    slack = jnp.minimum(tallies[giver] - 1, bound - tallies[sink]) // 2
    slack = jnp.where((giver == sequence[0]) | (sink == sequence[0]) | (tallies[sink] == 0), 0, jnp.maximum(slack, 0))
    moved = jax.random.randint(jax.random.fold_in(own, 4), (number_of // 2,), 0, 1 << 20) % (slack + 1)
    tallies = tallies.at[giver].add(-moved).at[sink].add(moved)
    labels = jnp.searchsorted(jnp.cumsum(tallies), jnp.arange(rows * top), side="right").astype(jnp.int32)
    table = labels.reshape(top, rows).T
    table = table[jax.random.permutation(jax.random.fold_in(own, 1), rows)]
    turn = jax.random.randint(jax.random.fold_in(own, 2), (rows, 1), 0, top)
    return jnp.take_along_axis(table, (jnp.arange(top)[None, :] + turn) % top, axis=1)


def shares(count, total, limit, skew, full):
    portions = [(1 << 20) // math.isqrt(grade ** skew) + 1 for grade in range(1, count + 1)]
    largest = limit if full else min(limit, max(-(-total // count), total * portions[0] // sum(portions)))
    least = 1 if total - largest >= count - 1 else 0
    holding, rest = [largest] + [least] * (count - 1), total - largest - least * (count - 1)
    while rest > 0:
        free = [i for i in range(1, count) if holding[i] < largest] or [i for i in range(1, count) if holding[i] < limit]
        mass, remaining = sum([portions[i] for i in free]), rest
        for i in free:
            addition = min(limit - holding[i], max(1, remaining * portions[i] // mass), rest)
            holding[i] = holding[i] + addition
            rest = rest - addition
    return np.array(holding)


def scatter_about(own_key, extent, deviation, reach, cuts=(), held_as=jnp.bfloat16):
    array = jax.random.normal(own_key, extent, jnp.float32) * deviation
    if len(cuts) > 0:
        array = level_of(own_key, extent, cuts, -0.22, 0.18) * array
    return jnp.clip(array, min=-reach, max=reach).astype(held_as)


def setup_inputs(seed: int = 0) -> dict:
    arg_keys = jax.random.split(jax.random.key(seed), 8)
    tokens = draw_tokens(jax.random.fold_in(arg_keys[7], 71), 0)
    norm_gain = jnp.clip(1.0 + 0.18 * jax.random.normal(arg_keys[1], (D,), jnp.float32), 0.099609375, 1.8984375).astype(jnp.bfloat16)
    routes_keys = jax.random.split(jax.random.fold_in(arg_keys[2], 1), TOKENS // TOK_DEV)
    routes_turns = jax.random.permutation(jax.random.fold_in(arg_keys[2], 3), TOKENS // TOK_DEV)
    routes = jax.vmap(lambda own, number: assign_block(jax.random.fold_in(arg_keys[2], 2), own, number, TOK_DEV, EXPERTS, TOPK, CAP, 2))(routes_keys, routes_turns).reshape((TOKENS, TOPK))
    route_weights = jnp.clip(0.05 + 0.95 * jax.random.uniform(arg_keys[3], (TOKENS, TOPK), jnp.float32) ** level_of(arg_keys[3], (TOKENS, TOPK), ((0, 8),), -0.2, 0.2), 0.05, 1.0)
    w_gate = scatter_about(arg_keys[4], (EXPERTS, D, FF), (D // 9) ** -0.5, 0.25, ((0, 8), (2, 4)))
    w_up = scatter_about(arg_keys[5], (EXPERTS, D, FF), (D // 9) ** -0.5, 0.25, ((0, 8), (2, 4)))
    w_down = scatter_about(arg_keys[6], (EXPERTS, FF, D), (16 * FF) ** -0.5, 0.0234375, ((0, 8), (1, 4)))
    return dict(tokens=tokens, norm_gain=norm_gain, routes=routes, route_weights=route_weights, w_gate=w_gate, w_up=w_up, w_down=w_down)


def reference(tokens, norm_gain, routes, route_weights, w_gate, w_up, w_down):
    values = tokens.astype(jnp.float32)
    scale = lax.rsqrt(lax.optimization_barrier(jnp.mean(values * values, axis=1, keepdims=True)) + 1e-05)
    normed = (values * scale * norm_gain.astype(jnp.float32)[None, :]).astype(jnp.bfloat16)
    blocks = N_TP
    rows = tokens.shape[0]

    def one_expert(carry, expert):
        gate_pre = jnp.dot(normed, w_gate[expert], preferred_element_type=jnp.float32)
        up_pre = jnp.dot(normed, w_up[expert], preferred_element_type=jnp.float32)
        gated = jnp.minimum(gate_pre, 7.0)
        upper = jnp.clip(up_pre, -7.0, 7.0)
        hidden = ((upper + 1.0) * gated * jax.nn.sigmoid(1.702 * gated)).astype(jnp.bfloat16)
        width = hidden.shape[1] // blocks
        hidden_blocks = hidden.reshape(rows, blocks, width).astype(jnp.float32)
        down_blocks = w_down[expert].reshape(blocks, width, -1).astype(jnp.float32)
        parts = jnp.einsum('tbf,bfd->btd', hidden_blocks, down_blocks).astype(jnp.bfloat16)
        parts = lax.optimization_barrier(parts).astype(jnp.float32)
        result = lax.optimization_barrier(jnp.sum(parts, axis=0)).astype(jnp.bfloat16)
        result = lax.optimization_barrier(result).astype(jnp.float32)
        weight = lax.optimization_barrier(jnp.sum(jnp.where(routes == expert, route_weights, 0.0), axis=1))
        return (carry + weight[:, None] * result, None)
    start = jnp.zeros(tokens.shape, jnp.float32)
    total, _ = lax.scan(one_expert, start, jnp.arange(EXPERTS, dtype=jnp.int32))
    return total.astype(jnp.bfloat16)
```

```python
import functools

import jax
import jax.numpy as jnp
from jax import lax
from jax.experimental import pallas as pl
from jax.experimental.pallas import tpu as pltpu
from jax.sharding import PartitionSpec as P

LANES = 128
AXES = ("ep", "tp")


def exchange(value, groups, n_tp, ep_xor, tp_xor):
    pairs = [
        (e * n_tp + t, (e ^ ep_xor) * n_tp + (t ^ tp_xor))
        for e in range(groups)
        for t in range(n_tp)
    ]
    return lax.ppermute(value, AXES, pairs)


def split_high_low(value):
    high = lax.reduce_precision(value, exponent_bits=8, mantissa_bits=7)
    return high, value - high


def expert_kernel(n_tp, groups, width, *refs):
    own = refs[:n_tp]
    other = refs[n_tp : 2 * n_tp]
    gate_ref, up_ref, down_ref, mine_ref, theirs_ref, x_ref, hidden_ref = refs[2 * n_tp :]
    t = lax.axis_index("tp")
    e = lax.axis_index("ep")
    rows = own[0].shape[0]
    hidden_width = gate_ref.shape[2]
    model = n_tp * width
    squares = jnp.zeros((2 * rows, 1), jnp.float32)
    for k in range(n_tp):
        x_ref[k, :rows, :] = own[k][:, :width]
        x_ref[k, rows:, :] = other[k][:, :width]
        meta = jnp.concatenate([own[k][:, width:], other[k][:, width:]], axis=0).astype(jnp.float32)
        lane = lax.broadcasted_iota(jnp.int32, meta.shape, 1)
        squares += jnp.sum(jnp.where(lane < 2, meta, 0.0), axis=1, keepdims=True)
        if k == 0:
            mask = (lane == 2 + e) | (lane == 2 + groups + e)
            weight = jnp.sum(jnp.where(mask, meta, 0.0), axis=1, keepdims=True)
    scale = lax.rsqrt(squares / model + 1e-05)

    tile = min(256, hidden_width)

    def first(j, carry):
        cols = pl.ds(pl.multiple_of(j * tile, tile), tile)
        gate = jnp.zeros((2 * rows, tile), jnp.float32)
        up = jnp.zeros((2 * rows, tile), jnp.float32)
        for k in range(n_tp):
            part = pl.ds(pl.multiple_of((t ^ k) * width, width), width)
            x = x_ref[k]
            gate += jnp.dot(x, gate_ref[0, part, cols], preferred_element_type=jnp.float32)
            up += jnp.dot(x, up_ref[0, part, cols], preferred_element_type=jnp.float32)
        gated = jnp.minimum(gate * scale, 7.0)
        upper = jnp.clip(up * scale, -7.0, 7.0)
        hidden = (upper + 1.0) * gated * jax.nn.sigmoid(1.702 * gated)
        hidden_ref[:, cols] = hidden.astype(jnp.bfloat16)
        return carry

    lax.fori_loop(0, hidden_width // tile, first, 0)

    out_tile = min(512, width)

    for k in range(n_tp):

        def second(j, carry, k=k):
            start = (t ^ k) * width + j * out_tile
            cols = pl.ds(pl.multiple_of(start, out_tile), out_tile)
            out = pl.ds(pl.multiple_of(j * out_tile, out_tile), out_tile)
            part = jnp.dot(
                hidden_ref[...], down_ref[0, :, cols], preferred_element_type=jnp.float32
            )
            part = part * weight
            mine_ref[k, :, out] = part[:rows]
            theirs_ref[k, :, out] = part[rows:].astype(jnp.bfloat16)
            return carry

        lax.fori_loop(0, width // out_tile, second, 0)


def run_expert(own, other, w_gate, w_up, w_down, groups, n_tp, width):
    rows = own[0].shape[0]
    hidden_width = w_gate.shape[2]
    whole = pl.BlockSpec(memory_space=pltpu.VMEM)
    flops = 2 * 2 * rows * (2 * w_gate.size + w_down.size)
    return pl.pallas_call(
        functools.partial(expert_kernel, n_tp, groups, width),
        out_shape=(
            jax.ShapeDtypeStruct((n_tp, rows, width), jnp.float32),
            jax.ShapeDtypeStruct((n_tp, rows, width), jnp.bfloat16),
        ),
        in_specs=[whole] * (2 * n_tp + 3),
        out_specs=(whole, whole),
        scratch_shapes=[
            pltpu.VMEM((n_tp, 2 * rows, width), jnp.bfloat16),
            pltpu.VMEM((2 * rows, hidden_width), jnp.bfloat16),
        ],
        cost_estimate=pl.CostEstimate(
            flops=flops, bytes_accessed=2 * 3 * w_gate.size, transcendentals=0
        ),
        compiler_params=pltpu.CompilerParams(vmem_limit_bytes=VMEM_LIMIT),
        name="expert",
    )(*own, *other, w_gate, w_up, w_down)


VMEM_LIMIT = 48 * 1024 * 1024


def shards(groups, n_tp, tokens, norm_gain, routes, route_weights, w_gate, w_up, w_down):
    tok_rows, width = tokens.shape
    n_z = groups // 2
    send = functools.partial(exchange, groups=groups, n_tp=n_tp)
    values = tokens.astype(jnp.float32)
    scaled = (values * norm_gain.astype(jnp.float32)[None, :]).astype(jnp.bfloat16)
    square = jnp.sum(values * values, axis=1, keepdims=True)
    experts = jnp.arange(groups, dtype=jnp.int32)
    weight = jnp.sum(
        jnp.where(routes[:, :, None] == experts[None, None, :], route_weights[:, :, None], 0.0),
        axis=1,
    )
    meta = [*split_high_low(square), *split_high_low(weight)]
    pad = -sum(m.shape[1] for m in meta) % LANES
    meta = jnp.concatenate([*meta, jnp.zeros((tok_rows, pad), jnp.float32)], axis=1)
    payload = jnp.concatenate([scaled, meta.astype(jnp.bfloat16)], axis=1)

    column = jnp.concatenate(
        [payload] + [send(payload, ep_xor=2 * k, tp_xor=0) for k in range(1, n_z)], axis=0
    )
    own = [column] + [send(column, ep_xor=0, tp_xor=k) for k in range(1, n_tp)]
    other = [send(piece, ep_xor=1, tp_xor=0) for piece in own]

    mine, theirs = run_expert(own, other, w_gate, w_up, w_down, groups, n_tp, width)

    paired = mine + send(theirs, ep_xor=1, tp_xor=0).astype(jnp.float32)
    total = paired[0]
    for k in range(1, n_tp):
        total += send(paired[k].astype(jnp.bfloat16), ep_xor=0, tp_xor=k).astype(jnp.float32)
    total = total.reshape(n_z, tok_rows, width)
    mixed = total[0]
    for k in range(1, n_z):
        mixed += send(total[k].astype(jnp.bfloat16), ep_xor=2 * k, tp_xor=0).astype(jnp.float32)
    return mixed.astype(jnp.bfloat16)


def solution(mesh):
    placed = (
        P("ep", "tp"),
        P("tp"),
        P("ep", None),
        P("ep", None),
        P("ep", None, "tp"),
        P("ep", None, "tp"),
        P("ep", "tp", None),
    )
    body = functools.partial(shards, mesh.shape["ep"], mesh.shape["tp"])
    return jax.shard_map(
        body, mesh=mesh, in_specs=placed, out_specs=P("ep", "tp"), check_vma=False
    )
```

```python
import functools

import jax
import jax.numpy as jnp
from jax import lax
from jax.experimental import pallas as pl
from jax.experimental.pallas import tpu as pltpu
from jax.sharding import PartitionSpec as P

LANES = 128
AXES = ("ep", "tp")


def exchange(value, groups, n_tp, ep_xor, tp_xor):
    pairs = [
        (e * n_tp + t, (e ^ ep_xor) * n_tp + (t ^ tp_xor))
        for e in range(groups)
        for t in range(n_tp)
    ]
    return lax.ppermute(value, AXES, pairs)


def split_high_low(value):
    high = lax.reduce_precision(value, exponent_bits=8, mantissa_bits=7)
    return high, value - high


def load_kernel(after_ref, source_ref, held_ref, sem):
    copy = pltpu.make_async_copy(source_ref, held_ref, sem)
    copy.start()
    copy.wait()


def load(weights, after, held):
    return pl.pallas_call(
        load_kernel,
        out_shape=pltpu.VMEM(weights.shape, weights.dtype),
        in_specs=[pl.BlockSpec(memory_space=pltpu.VMEM), pl.BlockSpec(memory_space=pltpu.HBM)],
        out_specs=pl.BlockSpec(memory_space=pltpu.VMEM),
        scratch_shapes=[pltpu.SemaphoreType.DMA],
        cost_estimate=pl.CostEstimate(
            flops=LOAD_FLOPS * weights.size, bytes_accessed=4 * weights.size, transcendentals=0
        ),
        compiler_params=pltpu.CompilerParams(vmem_limit_bytes=VMEM - (2 * held + 1) * weights.size - 3 * MIB),
        name="load",
    )(after, weights)


def expert_kernel(n_tp, groups, width, *refs):
    own = refs[:n_tp]
    other = refs[n_tp : 2 * n_tp]
    gate_ref, up_ref, down_hbm, mine_ref, theirs_ref, x_ref, hidden_ref, down_ref, sem = refs[
        2 * n_tp :
    ]
    down_copy = pltpu.make_async_copy(down_hbm, down_ref, sem)
    down_copy.start()
    t = lax.axis_index("tp")
    e = lax.axis_index("ep")
    rows = own[0].shape[0]
    hidden_width = gate_ref.shape[2]
    model = n_tp * width
    squares = jnp.zeros((2 * rows, 1), jnp.float32)
    for k in range(n_tp):
        x_ref[k, :rows, :] = own[k][:, :width]
        x_ref[k, rows:, :] = other[k][:, :width]
        meta = jnp.concatenate([own[k][:, width:], other[k][:, width:]], axis=0).astype(jnp.float32)
        lane = lax.broadcasted_iota(jnp.int32, meta.shape, 1)
        squares += jnp.sum(jnp.where(lane < 2, meta, 0.0), axis=1, keepdims=True)
        if k == 0:
            mask = (lane == 2 + e) | (lane == 2 + groups + e)
            weight = jnp.sum(jnp.where(mask, meta, 0.0), axis=1, keepdims=True)
    scale = lax.rsqrt(squares / model + 1e-05)

    tile = min(256, hidden_width)

    def first(j, carry):
        cols = pl.ds(pl.multiple_of(j * tile, tile), tile)
        gate = jnp.zeros((2 * rows, tile), jnp.float32)
        up = jnp.zeros((2 * rows, tile), jnp.float32)
        for k in range(n_tp):
            part = pl.ds(pl.multiple_of((t ^ k) * width, width), width)
            x = x_ref[k]
            gate += jnp.dot(x, gate_ref[0, part, cols], preferred_element_type=jnp.float32)
            up += jnp.dot(x, up_ref[0, part, cols], preferred_element_type=jnp.float32)
        gated = jnp.minimum(gate * scale, 7.0)
        upper = jnp.clip(up * scale, -7.0, 7.0)
        hidden = (upper + 1.0) * gated * jax.nn.sigmoid(1.702 * gated)
        hidden_ref[:, cols] = hidden.astype(jnp.bfloat16)
        return carry

    lax.fori_loop(0, hidden_width // tile, first, 0)

    out_tile = min(512, width)
    down_copy.wait()

    for k in range(n_tp):

        def second(j, carry, k=k):
            start = (t ^ k) * width + j * out_tile
            cols = pl.ds(pl.multiple_of(start, out_tile), out_tile)
            out = pl.ds(pl.multiple_of(j * out_tile, out_tile), out_tile)
            part = jnp.dot(
                hidden_ref[...], down_ref[0, :, cols], preferred_element_type=jnp.float32
            )
            part = part * weight
            mine_ref[k, :, out] = part[:rows]
            theirs_ref[k, :, out] = part[rows:].astype(jnp.bfloat16)
            return carry

        lax.fori_loop(0, width // out_tile, second, 0)


def run_expert(own, other, w_gate, w_up, w_down, groups, n_tp, width):
    rows = own[0].shape[0]
    hidden_width = w_gate.shape[2]
    whole = pl.BlockSpec(memory_space=pltpu.VMEM)
    flops = 2 * 2 * rows * (2 * w_gate.size + w_down.size)
    return pl.pallas_call(
        functools.partial(expert_kernel, n_tp, groups, width),
        out_shape=(
            jax.ShapeDtypeStruct((n_tp, rows, width), jnp.float32),
            jax.ShapeDtypeStruct((n_tp, rows, width), jnp.bfloat16),
        ),
        in_specs=[whole] * (2 * n_tp + 2) + [pl.BlockSpec(memory_space=pltpu.HBM)],
        out_specs=(whole, whole),
        scratch_shapes=[
            pltpu.VMEM((n_tp, 2 * rows, width), jnp.bfloat16),
            pltpu.VMEM((2 * rows, hidden_width), jnp.bfloat16),
            pltpu.VMEM(w_down.shape, w_down.dtype),
            pltpu.SemaphoreType.DMA,
        ],
        cost_estimate=pl.CostEstimate(
            flops=flops, bytes_accessed=2 * 3 * w_gate.size, transcendentals=0
        ),
        compiler_params=pltpu.CompilerParams(vmem_limit_bytes=VMEM_LIMIT),
        name="expert",
    )(*own, *other, w_gate, w_up, w_down)


MIB = 1024 * 1024
VMEM = 63 * MIB
VMEM_LIMIT = 32 * MIB
LOAD_FLOPS = 2000


def shards(groups, n_tp, tokens, norm_gain, routes, route_weights, w_gate, w_up, w_down):
    tok_rows, width = tokens.shape
    n_z = groups // 2
    send = functools.partial(exchange, groups=groups, n_tp=n_tp)
    values = tokens.astype(jnp.float32)
    scaled = (values * norm_gain.astype(jnp.float32)[None, :]).astype(jnp.bfloat16)
    square = jnp.sum(values * values, axis=1, keepdims=True)
    experts = jnp.arange(groups, dtype=jnp.int32)
    weight = jnp.sum(
        jnp.where(routes[:, :, None] == experts[None, None, :], route_weights[:, :, None], 0.0),
        axis=1,
    )
    meta = [*split_high_low(square), *split_high_low(weight)]
    pad = -sum(m.shape[1] for m in meta) % LANES
    meta = jnp.concatenate([*meta, jnp.zeros((tok_rows, pad), jnp.float32)], axis=1)
    payload = jnp.concatenate([scaled, meta.astype(jnp.bfloat16)], axis=1)

    gate_held = load(w_gate, payload, 1)
    column = jnp.concatenate(
        [payload] + [send(payload, ep_xor=2 * k, tp_xor=0) for k in range(1, n_z)], axis=0
    )
    column, gate_held = lax.optimization_barrier((column, gate_held))
    up_held = load(w_up, column, 2)
    own = [column] + [send(column, ep_xor=0, tp_xor=k) for k in range(1, n_tp)]
    other = [send(piece, ep_xor=1, tp_xor=0) for piece in own]

    mine, theirs = run_expert(own, other, gate_held, up_held, w_down, groups, n_tp, width)

    paired = mine + send(theirs, ep_xor=1, tp_xor=0).astype(jnp.float32)
    total = paired[0]
    for k in range(1, n_tp):
        total += send(paired[k].astype(jnp.bfloat16), ep_xor=0, tp_xor=k).astype(jnp.float32)
    total = total.reshape(n_z, tok_rows, width)
    mixed = total[0]
    for k in range(1, n_z):
        mixed += send(total[k].astype(jnp.bfloat16), ep_xor=2 * k, tp_xor=0).astype(jnp.float32)
    return mixed.astype(jnp.bfloat16)


def solution(mesh):
    placed = (
        P("ep", "tp"),
        P("tp"),
        P("ep", None),
        P("ep", None),
        P("ep", None, "tp"),
        P("ep", None, "tp"),
        P("ep", "tp", None),
    )
    body = functools.partial(shards, mesh.shape["ep"], mesh.shape["tp"])
    return jax.shard_map(
        body, mesh=mesh, in_specs=placed, out_specs=P("ep", "tp"), check_vma=False
    )
```

```python
import functools

import jax
import jax.numpy as jnp
from jax import lax
from jax.experimental import pallas as pl
from jax.experimental.pallas import tpu as pltpu
from jax.sharding import PartitionSpec as P

LANES = 128
AXES = ("ep", "tp")


def exchange(value, groups, n_tp, ep_xor, tp_xor):
    pairs = [
        (e * n_tp + t, (e ^ ep_xor) * n_tp + (t ^ tp_xor))
        for e in range(groups)
        for t in range(n_tp)
    ]
    return lax.ppermute(value, AXES, pairs)


def prepare_kernel(tokens_ref, gain_ref, weight_ref, payload_ref):
    width = tokens_ref.shape[1]
    groups = weight_ref.shape[1]
    values = tokens_ref[...].astype(jnp.float32)
    payload_ref[:, :width] = (values * gain_ref[...].astype(jnp.float32)).astype(jnp.bfloat16)
    extra = payload_ref.shape[1] - width
    lane = lax.broadcasted_iota(jnp.int32, (values.shape[0], extra), 1)
    place = jnp.where(lane < extra // 2, lane, lane - extra // 2)
    meta = jnp.where(place == 0, jnp.sum(values * values, axis=1, keepdims=True), 0.0)
    for e in range(groups):
        meta = jnp.where(place == 1 + e, weight_ref[:, e : e + 1], meta)
    high = meta.astype(jnp.bfloat16).astype(jnp.float32)
    payload_ref[:, width:] = jnp.where(lane < extra // 2, high, meta - high).astype(jnp.bfloat16)


def prepare(tokens, gain, weight):
    extra = 2 * (-(-(1 + weight.shape[1]) // (LANES // 2)) * (LANES // 2))
    return pl.pallas_call(
        prepare_kernel,
        out_shape=jax.ShapeDtypeStruct((tokens.shape[0], tokens.shape[1] + extra), jnp.bfloat16),
        in_specs=[pl.BlockSpec(memory_space=pltpu.VMEM)] * 3,
        out_specs=pl.BlockSpec(memory_space=pltpu.VMEM),
        compiler_params=pltpu.CompilerParams(vmem_limit_bytes=4 * MIB),
        name="prepare",
    )(tokens, gain.reshape(1, -1), weight)


def load_kernel(halves, after_ref, *refs):
    n = len(halves)
    sources, held, sem = refs[:n], refs[n : 2 * n], refs[2 * n]
    copies = []
    for i, half in enumerate(halves):
        cols = pl.ds(half * held[i].shape[2], held[i].shape[2])
        copies.append(pltpu.make_async_copy(sources[i].at[:, :, cols], held[i], sem.at[i]))
        copies[-1].start()
    for copy in copies:
        copy.wait()


def load(sources, halves, after, held, parts):
    e, d, f = sources[0].shape
    piece = e * d * f // parts
    n = len(sources)
    return pl.pallas_call(
        functools.partial(load_kernel, halves),
        out_shape=[pltpu.VMEM((e, d, f // parts), w.dtype) for w in sources],
        in_specs=[pl.BlockSpec(memory_space=pl.ANY)]
        + [pl.BlockSpec(memory_space=pltpu.HBM)] * n,
        out_specs=[pl.BlockSpec(memory_space=pltpu.VMEM)] * n,
        scratch_shapes=[pltpu.SemaphoreType.DMA((n,))],
        cost_estimate=pl.CostEstimate(
            flops=LOAD_FLOPS * piece * n, bytes_accessed=4 * piece * n, transcendentals=0
        ),
        compiler_params=pltpu.CompilerParams(
            vmem_limit_bytes=VMEM - 2 * (held + n) * piece - 9 * MIB
        ),
        name="load",
    )(after, *sources)


def expert_kernel(n_tp, groups, width, *refs):
    own = refs[:n_tp]
    other = refs[n_tp : 2 * n_tp]
    rest = refs[2 * n_tp :]
    parts = (len(rest) - 7) // 2
    gates, ups = rest[:parts], rest[parts : 2 * parts]
    down_hbm, mine_ref, theirs_ref, x_ref, hidden_ref, down_ref, sem = rest[2 * parts :]
    down_copy = pltpu.make_async_copy(down_hbm, down_ref, sem)
    down_copy.start()
    t = lax.axis_index("tp")
    e = lax.axis_index("ep")
    rows = own[0].shape[0]
    part_width = gates[0].shape[2]
    model = n_tp * width
    squares = jnp.zeros((2 * rows, 1), jnp.float32)
    for k in range(n_tp):
        x_ref[k, :rows, :] = own[k][:, :width]
        x_ref[k, rows:, :] = other[k][:, :width]
        meta = jnp.concatenate([own[k][:, width:], other[k][:, width:]], axis=0).astype(jnp.float32)
        lane = lax.broadcasted_iota(jnp.int32, meta.shape, 1)
        half = meta.shape[1] // 2
        squares += jnp.sum(jnp.where((lane == 0) | (lane == half), meta, 0.0), axis=1, keepdims=True)
        if k == 0:
            mask = (lane == 1 + e) | (lane == half + 1 + e)
            weight = jnp.sum(jnp.where(mask, meta, 0.0), axis=1, keepdims=True)
    scale = lax.rsqrt(squares / model + 1e-05)

    tile = min(256, part_width)

    def first(j, carry, gate_ref, up_ref, base):
        cols = pl.ds(pl.multiple_of(j * tile, tile), tile)
        gate = jnp.zeros((2 * rows, tile), jnp.float32)
        up = jnp.zeros((2 * rows, tile), jnp.float32)
        for k in range(n_tp):
            part = pl.ds(pl.multiple_of((t ^ k) * width, width), width)
            x = x_ref[k]
            gate += jnp.dot(x, gate_ref[0, part, cols], preferred_element_type=jnp.float32)
            up += jnp.dot(x, up_ref[0, part, cols], preferred_element_type=jnp.float32)
        gated = jnp.minimum(gate * scale, 7.0)
        upper = jnp.clip(up * scale, -7.0, 7.0)
        hidden = (upper + 1.0) * gated * jax.nn.sigmoid(1.702 * gated)
        out = pl.ds(pl.multiple_of(base + j * tile, tile), tile)
        hidden_ref[:, out] = hidden.astype(jnp.bfloat16)
        return carry

    for i in range(parts):
        step = functools.partial(
            first, gate_ref=gates[i], up_ref=ups[i], base=i * part_width
        )
        lax.fori_loop(0, part_width // tile, step, 0)

    out_tile = min(512, width)
    down_copy.wait()

    for k in range(n_tp):

        def second(j, carry, k=k):
            start = (t ^ k) * width + j * out_tile
            cols = pl.ds(pl.multiple_of(start, out_tile), out_tile)
            out = pl.ds(pl.multiple_of(j * out_tile, out_tile), out_tile)
            part = jnp.dot(
                hidden_ref[...], down_ref[0, :, cols], preferred_element_type=jnp.float32
            )
            part = part * weight
            mine_ref[k, :, out] = part[:rows]
            theirs_ref[k, :, out] = part[rows:].astype(jnp.bfloat16)
            return carry

        lax.fori_loop(0, width // out_tile, second, 0)


def run_expert(own, other, gates, ups, w_down, groups, n_tp, width):
    rows = own[0].shape[0]
    hidden_width = w_down.shape[1]
    whole = pl.BlockSpec(memory_space=pltpu.VMEM)
    flops = 2 * 2 * rows * 3 * w_down.size
    return pl.pallas_call(
        functools.partial(expert_kernel, n_tp, groups, width),
        out_shape=(
            jax.ShapeDtypeStruct((n_tp, rows, width), jnp.float32),
            jax.ShapeDtypeStruct((n_tp, rows, width), jnp.bfloat16),
        ),
        in_specs=[whole] * (2 * n_tp + 2 * len(gates)) + [pl.BlockSpec(memory_space=pltpu.HBM)],
        out_specs=(whole, whole),
        scratch_shapes=[
            pltpu.VMEM((n_tp, 2 * rows, width), jnp.bfloat16),
            pltpu.VMEM((2 * rows, hidden_width), jnp.bfloat16),
            pltpu.VMEM(w_down.shape, w_down.dtype),
            pltpu.SemaphoreType.DMA,
        ],
        cost_estimate=pl.CostEstimate(
            flops=flops, bytes_accessed=6 * w_down.size, transcendentals=0
        ),
        compiler_params=pltpu.CompilerParams(vmem_limit_bytes=VMEM_LIMIT),
        name="expert",
    )(*own, *other, *gates, *ups, w_down)


MIB = 1024 * 1024
VMEM = 63 * MIB
VMEM_LIMIT = 32 * MIB
LOAD_FLOPS = 2000


def shards(groups, n_tp, tokens, norm_gain, routes, route_weights, w_gate, w_up, w_down):
    tok_rows, width = tokens.shape
    n_z = groups // 2
    send = functools.partial(exchange, groups=groups, n_tp=n_tp)
    experts = jnp.arange(groups, dtype=jnp.int32)
    weight = jnp.sum(
        jnp.where(routes[:, :, None] == experts[None, None, :], route_weights[:, :, None], 0.0),
        axis=1,
    )
    payload = prepare(tokens, norm_gain, weight)

    parts = 2 if w_gate.shape[2] % (2 * LANES) == 0 else 1
    arrived = [send(payload, ep_xor=2 * k, tp_xor=0) for k in range(1, n_z)]
    first = list(load([w_gate], [0], payload, 0, parts))
    column = jnp.concatenate([payload, *arrived], axis=0)
    column, first[0] = lax.optimization_barrier((column, first[0]))

    rest = [(w, i) for i in range(parts) for w in (w_gate, w_up)][1:]
    arrived = [send(column, ep_xor=0, tp_xor=k) for k in range(1, n_tp)]
    swapped = send(column, ep_xor=1, tp_xor=0)
    later = list(load([w for w, _ in rest], [i for _, i in rest], column, 1, parts))
    arrived = [lax.optimization_barrier((piece, later[0]))[0] for piece in arrived]
    own = [column, *arrived]
    other = [swapped] + [send(piece, ep_xor=1, tp_xor=0) for piece in arrived]
    held = [first[0], *later]

    mine, theirs = run_expert(own, other, held[0::2], held[1::2], w_down, groups, n_tp, width)

    paired = mine + send(theirs, ep_xor=1, tp_xor=0).astype(jnp.float32)
    total = paired[0]
    for k in range(1, n_tp):
        total += send(paired[k].astype(jnp.bfloat16), ep_xor=0, tp_xor=k).astype(jnp.float32)
    total = total.reshape(n_z, tok_rows, width)
    mixed = total[0]
    for k in range(1, n_z):
        mixed += send(total[k].astype(jnp.bfloat16), ep_xor=2 * k, tp_xor=0).astype(jnp.float32)
    return mixed.astype(jnp.bfloat16)


def solution(mesh):
    placed = (
        P("ep", "tp"),
        P("tp"),
        P("ep", None),
        P("ep", None),
        P("ep", None, "tp"),
        P("ep", None, "tp"),
        P("ep", "tp", None),
    )
    body = functools.partial(shards, mesh.shape["ep"], mesh.shape["tp"])
    return jax.shard_map(
        body, mesh=mesh, in_specs=placed, out_specs=P("ep", "tp"), check_vma=False
    )
```
